32 devices in a mesh: sp: 8 (over z, y), tp: 4 (over x, core).
Axes of the slice: x: 2, y: 2, z: 4, core: 2. Of those that a mesh axis runs over, the one named last changes fastest.
Arguments:
- resid_in: bfloat16 [2048, 2048], P('sp'), may hold values from -6 to 6
- query_latent: bfloat16 [2048, 768], P('sp'), may hold values from -6 to 6
- kv_latent: bfloat16 [2048, 512], P('sp'), may hold values from -6 to 6
- rotary_key: bfloat16 [2048, 64], P('sp'), may hold values from -200 to 200
- query_gain: float32 [768], replicated, may hold values from 0.1 to 1.9
- kv_gain: float32 [512], replicated, may hold values from 0.1 to 1.9
- w_query_plain: bfloat16 [768, 2048], P(None, 'tp'), may hold values from -0.875 to 0.875
- w_query_rotary: bfloat16 [768, 1024], P(None, 'tp'), may hold values from -0.875 to 0.875
- w_key_plain: bfloat16 [512, 2048], P(None, 'tp'), may hold values from -0.25 to 0.25
- w_value: bfloat16 [512, 2048], P(None, 'tp'), may hold values from -0.25 to 0.25
- w_output: bfloat16 [2048, 2048], P('tp'), may hold values from -0.125 to 0.125
- ffn_gain: float32 [2048], replicated, may hold values from 0.1 to 1.9
- w_gate: bfloat16 [2048, 5632], P('sp', 'tp'), may hold values from -0.125 to 0.125
- w_up: bfloat16 [2048, 5632], P('sp', 'tp'), may hold values from -0.125 to 0.125
- w_down: bfloat16 [5632, 2048], P('tp', 'sp'), may hold values from -0.078125 to 0.078125
Outputs:
- resid_out: bfloat16 [2048, 2048], P(('sp', 'tp'))
The draws below stay inside these ranges and needn't reach their ends.
All inputs are finite; a program needn't handle non-finite values.
Results may differ from the reference program's by a relative error of at most 0.014.
The reference program's roundings to bfloat16 on the way count: a program that leaves them out, or rounds other values in their place, can miss the bound.
Values may be sent and summed in bfloat16 or wider, within the bound.
A program may use at most 192 MiB of HBM per device.

```python
import jax
import jax.numpy as jnp
from jax import lax

D = 2048
HEADS = 16
QR = 768
KVR = 512
NOPE = 128
ROPE = 64
VDIM = 128
FF = 5632
TOK_DEV = 256
SEQ = 2048


def draw_rotary_key(key, part):
    first = jax.random.fold_in(jax.random.fold_in(key, 11), 0)
    base = jnp.clip(jax.random.normal(first, (SEQ, ROPE), jnp.float32), -5.0, 5.0)
    return base.astype(jnp.bfloat16)


def shard_levels(own_key, shape, cuts, smallest, top_value):
    factor_of = 1.0
    for dim, blocks in cuts:
        draws = jax.random.uniform(jax.random.fold_in(jax.random.fold_in(own_key, 6), dim), (blocks,), jnp.float32, smallest / len(cuts), top_value / len(cuts))
        factor_of = factor_of * jnp.repeat(jnp.exp(draws), shape[dim] // blocks).reshape((-1,) + (1,) * (len(shape) - 1 - dim))
    return factor_of


def normal_values(stream_key, dims, spread, most, cuts=(), kind=jnp.bfloat16):
    drawn = jax.random.normal(stream_key, dims, jnp.float32) * spread
    if len(cuts) > 0:
        drawn = shard_levels(stream_key, dims, cuts, -0.22, 0.18) * drawn
    return jnp.clip(drawn, min=-most, max=most).astype(kind)


def setup_inputs(seed: int = 0) -> dict:
    key_of = jax.random.split(jax.random.key(seed), 16)
    resid_in = normal_values(key_of[0], (SEQ, D), 1.0, 6.0, ((0, 8),))
    query_latent = normal_values(key_of[1], (SEQ, QR), 1.0, 6.0, ((0, 8),))
    kv_latent = normal_values(key_of[2], (SEQ, KVR), 1.0, 6.0, ((0, 8),))
    rotary_key = draw_rotary_key(jax.random.fold_in(key_of[15], 71), 0)
    query_gain = jnp.clip(1.0 + 0.18 * jax.random.normal(key_of[4], (QR,), jnp.float32), 0.1, 1.9)
    kv_gain = jnp.clip(1.0 + 0.18 * jax.random.normal(key_of[5], (KVR,), jnp.float32), 0.1, 1.9)
    w_query_plain = normal_values(key_of[6], (QR, HEADS * NOPE), (QR // 16) ** -0.5, 0.875, ((1, 4),))
    w_query_rotary = normal_values(key_of[7], (QR, HEADS * ROPE), (QR // 16) ** -0.5, 0.875, ((1, 4),))
    w_key_plain = normal_values(key_of[8], (KVR, HEADS * NOPE), KVR ** -0.5, 0.25, ((1, 4),))
    w_value = normal_values(key_of[9], (KVR, HEADS * VDIM), KVR ** -0.5, 0.25, ((1, 4),))
    w_output = normal_values(key_of[10], (HEADS * VDIM, D), (HEADS * VDIM) ** -0.5, 0.125, ((0, 4),))
    ffn_gain = jnp.clip(1.0 + 0.18 * jax.random.normal(key_of[11], (D,), jnp.float32), 0.1, 1.9)
    w_gate = normal_values(key_of[12], (D, FF), D ** -0.5, 0.125, ((0, 8), (1, 4)))
    w_up = normal_values(key_of[13], (D, FF), D ** -0.5, 0.125, ((0, 8), (1, 4)))
    w_down = normal_values(key_of[14], (FF, D), FF ** -0.5, 0.078125, ((0, 4), (1, 8)))
    return dict(resid_in=resid_in, query_latent=query_latent, kv_latent=kv_latent, rotary_key=rotary_key, query_gain=query_gain, kv_gain=kv_gain, w_query_plain=w_query_plain, w_query_rotary=w_query_rotary, w_key_plain=w_key_plain, w_value=w_value, w_output=w_output, ffn_gain=ffn_gain, w_gate=w_gate, w_up=w_up, w_down=w_down)


def normed(values, gain):
    wide = values.astype(jnp.float32)
    return wide * lax.rsqrt(lax.optimization_barrier(jnp.mean(wide * wide, axis=-1, keepdims=True)) + 1e-06) * gain.astype(jnp.float32)

def rotate(values, cosine, sine):
    half = values.shape[-1] // 2
    first = values[..., :half]
    second = values[..., half:]
    return jnp.concatenate([first * cosine - second * sine, second * cosine + first * sine], axis=-1)

def reference(resid_in, query_latent, kv_latent, rotary_key, query_gain, kv_gain, w_query_plain, w_query_rotary, w_key_plain, w_value, w_output, ffn_gain, w_gate, w_up, w_down):
    length = resid_in.shape[0]
    position = jnp.arange(length, dtype=jnp.float32)
    freq = 10000.0 ** (-jnp.arange(0, ROPE, 2, dtype=jnp.float32) / ROPE)
    angle = position[:, None] * freq[None, :]
    cosine = jnp.cos(angle)
    sine = jnp.sin(angle)
    q_norm = normed(query_latent, query_gain).astype(jnp.bfloat16)
    kv_norm = normed(kv_latent, kv_gain).astype(jnp.bfloat16)
    key_rot = rotate(rotary_key.astype(jnp.float32), cosine, sine).astype(jnp.bfloat16)
    q_plain = jnp.dot(q_norm, w_query_plain, preferred_element_type=jnp.float32).astype(jnp.bfloat16).reshape(length, HEADS, NOPE)
    q_raw = jnp.dot(q_norm, w_query_rotary, preferred_element_type=jnp.float32).reshape(length, HEADS, ROPE)
    q_rot = rotate(q_raw, cosine[:, None, :], sine[:, None, :]).astype(jnp.bfloat16)
    k_plain = jnp.dot(kv_norm, w_key_plain, preferred_element_type=jnp.float32).astype(jnp.bfloat16).reshape(length, HEADS, NOPE)
    values = jnp.dot(kv_norm, w_value, preferred_element_type=jnp.float32).astype(jnp.bfloat16).reshape(length, HEADS, VDIM)
    k_wide = k_plain.astype(jnp.float32)
    v_wide = values.astype(jnp.float32)
    r_wide = key_rot.astype(jnp.float32)
    scale = (NOPE + ROPE) ** (-0.5)
    blocks = length // TOK_DEV

    def attend(pair):
        q_a, q_b = pair
        score = (jnp.einsum('qhd,khd->hqk', q_a.astype(jnp.float32), k_wide) + jnp.einsum('qhr,kr->hqk', q_b.astype(jnp.float32), r_wide)) * scale
        top = lax.optimization_barrier(jnp.max(score, axis=-1, keepdims=True))
        weight = jnp.exp(score - top)
        total = lax.optimization_barrier(jnp.sum(weight, axis=-1))
        mixed = jnp.einsum('hqk,khd->qhd', weight.astype(jnp.bfloat16).astype(jnp.float32), v_wide)
        return (mixed / jnp.transpose(total)[:, :, None]).astype(jnp.bfloat16)
    attn = lax.map(attend, (q_plain.reshape(blocks, TOK_DEV, HEADS, NOPE), q_rot.reshape(blocks, TOK_DEV, HEADS, ROPE)))
    attn = attn.reshape(length, HEADS * VDIM)
    mid = resid_in.astype(jnp.float32) + jnp.dot(attn, w_output, preferred_element_type=jnp.float32)
    h_norm = normed(mid, ffn_gain).astype(jnp.bfloat16)
    gate = jnp.dot(h_norm, w_gate, preferred_element_type=jnp.float32)
    upper = jnp.dot(h_norm, w_up, preferred_element_type=jnp.float32)
    hidden = (jax.nn.silu(gate) * upper).astype(jnp.bfloat16)
    return (mid + jnp.dot(hidden, w_down, preferred_element_type=jnp.float32)).astype(jnp.bfloat16)
```

```python
import functools

import jax
import jax.numpy as jnp
from jax import lax
from jax.experimental import pallas as pl
from jax.experimental.pallas import tpu as pltpu
from jax.sharding import PartitionSpec as P

NOPE = 128
ROPE = 64
VDIM = 128
MESH = pl.DeviceIdType.MESH


def normed(values, gain):
    wide = values.astype(jnp.float32)
    return wide * lax.rsqrt(jnp.mean(wide * wide, axis=-1, keepdims=True) + 1e-06) * gain


def rotate(values, cosine, sine):
    half = values.shape[-1] // 2
    first = values[..., :half]
    second = values[..., half:]
    return jnp.concatenate(
        [first * cosine - second * sine, second * cosine + first * sine], axis=-1
    )


class Plan:
    def __init__(self, sp, tp):
        self.sp, self.tp = sp, tp
        self.z = 4 if sp % 4 == 0 else 1
        self.r = sp // self.z
        self.c = 2 if tp % 2 == 0 else 1
        self.x = tp // self.c

    def sizes(self):
        return {"z": self.z, "r": self.r, "x": self.x, "c": self.c}

    def here(self):
        s, t = lax.axis_index("sp"), lax.axis_index("tp")
        return {"z": s // self.r, "r": lax.rem(s, self.r), "x": t // self.c, "c": lax.rem(t, self.c)}

    def device(self, at):
        return {"sp": at["z"] * self.r + at["r"], "tp": at["x"] * self.c + at["c"]}

    def shifted(self, at, axis, by):
        size = self.sizes()[axis]
        return {**at, axis: lax.rem(at[axis] + (by % size), size)}


def meet(plan, here, axes):
    barrier = pltpu.get_barrier_semaphore()
    count = 0
    for axis in axes:
        for k in range(1, plan.sizes()[axis]):
            pl.semaphore_signal(
                barrier,
                inc=1,
                device_id=plan.device(plan.shifted(here, axis, k)),
                device_id_type=MESH,
            )
            count += 1
    if count:
        pl.semaphore_wait(barrier, count)


def gather_body(plan, axes, order, x_ref, o_ref, send_a, recv_a, send_b, recv_b, send_c, recv_c, own):
    here = plan.here()
    sizes = plan.sizes()
    a, b, c = axes
    na, nb, nc = (sizes[axis] for axis in axes)

    def slot(at):
        index = 0
        for axis in order:
            index = index * sizes[axis] + at[axis]
        return index

    meet(plan, here, axes)

    def send(src, block, axis, by, sem_s, sem_r):
        copy = pltpu.make_async_remote_copy(
            src_ref=src,
            dst_ref=o_ref.at[slot(block)],
            send_sem=sem_s,
            recv_sem=sem_r,
            device_id=plan.device(plan.shifted(here, axis, by)),
            device_id_type=MESH,
        )
        copy.start()
        return copy

    mine = pltpu.make_async_copy(x_ref, o_ref.at[slot(here)], own)
    mine.start()
    first = {}
    for k in range(1, na):
        first[k] = send(x_ref, here, a, k, send_a.at[k], recv_a.at[k])
    second, third = {}, {}
    for k in range(na):
        block = plan.shifted(here, a, -k)
        if k:
            first[k].wait_recv()
        src = o_ref.at[slot(block)] if k else x_ref
        for j in range(1, nb):
            second[k, j] = send(src, block, b, j, send_b.at[k, j], recv_b.at[k, j])
        for l in range(1, nc):
            third[k, 0, l] = send(src, block, c, l, send_c.at[k, 0, l], recv_c.at[k, 0, l])
    for k in range(na):
        for j in range(1, nb):
            second[k, j].wait_recv()
            block = plan.shifted(plan.shifted(here, a, -k), b, -j)
            for l in range(1, nc):
                third[k, j, l] = send(
                    o_ref.at[slot(block)], block, c, l, send_c.at[k, j, l], recv_c.at[k, j, l]
                )
    for copy in third.values():
        copy.wait_recv()
    for copy in [*first.values(), *second.values(), *third.values()]:
        copy.wait_send()
    mine.wait()


def gather(plan, block, axes, order, ident):
    na, nb, nc = (plan.sizes()[axis] for axis in axes)
    count = na * nb * nc
    dma = pltpu.SemaphoreType.DMA
    out = pl.pallas_call(
        functools.partial(gather_body, plan, axes, order),
        out_shape=jax.ShapeDtypeStruct((count,) + block.shape, block.dtype),
        in_specs=[pl.BlockSpec(memory_space=pl.ANY)],
        out_specs=pl.BlockSpec(memory_space=pl.ANY),
        scratch_shapes=[
            dma((na,)),
            dma((na,)),
            dma((na, nb)),
            dma((na, nb)),
            dma((na, nb, nc)),
            dma((na, nb, nc)),
            dma,
        ],
        compiler_params=pltpu.CompilerParams(collective_id=ident, has_side_effects=True),
        cost_estimate=pl.CostEstimate(
            flops=20_000_000_000, bytes_accessed=2 * count * block.size, transcendentals=0
        ),
    )(block)
    return out.reshape((count * block.shape[0],) + block.shape[1:])


def swap_body(plan, x_ref, o_ref, send_sem, recv_sem, own):
    tp = plan.tp
    s, t = lax.axis_index("sp"), lax.axis_index("tp")
    barrier = pltpu.get_barrier_semaphore()
    for k in range(1, tp):
        pl.semaphore_signal(
            barrier, inc=1, device_id={"sp": s, "tp": lax.rem(t + k, tp)}, device_id_type=MESH
        )
    pl.semaphore_wait(barrier, tp - 1)
    copies = []
    for k in range(1, tp):
        to = lax.rem(t + k, tp)
        copy = pltpu.make_async_remote_copy(
            src_ref=x_ref.at[to],
            dst_ref=o_ref.at[t],
            send_sem=send_sem.at[k],
            recv_sem=recv_sem.at[k],
            device_id={"sp": s, "tp": to},
            device_id_type=MESH,
        )
        copy.start()
        copies.append(copy)
    mine = pltpu.make_async_copy(x_ref.at[t], o_ref.at[t], own)
    mine.start()
    for copy in copies:
        copy.wait()
    mine.wait()


def swap(plan, blocks, ident):
    dma = pltpu.SemaphoreType.DMA
    return pl.pallas_call(
        functools.partial(swap_body, plan),
        out_shape=jax.ShapeDtypeStruct(blocks.shape, blocks.dtype),
        in_specs=[pl.BlockSpec(memory_space=pl.ANY)],
        out_specs=pl.BlockSpec(memory_space=pl.ANY),
        scratch_shapes=[dma((plan.tp,)), dma((plan.tp,)), dma],
        compiler_params=pltpu.CompilerParams(collective_id=ident, has_side_effects=True),
        cost_estimate=pl.CostEstimate(
            flops=10_000_000_000, bytes_accessed=4 * blocks.size, transcendentals=0
        ),
    )(blocks)


def reduce_body(
    plan, p_ref, m_ref, o_ref, got_c, sum_c, got_x, sum_x, got_z, s_c, r_c, s_x, r_x, s_z, r_z
):
    nz, nx, nc = plan.z, plan.x, plan.c
    here = plan.here()
    z, x, c = here["z"], here["x"], here["c"]
    meet(plan, here, ("z", "x", "c"))

    def send(src, dst, axis, by, sem_s, sem_r):
        copy = pltpu.make_async_remote_copy(
            src_ref=src,
            dst_ref=dst,
            send_sem=sem_s,
            recv_sem=sem_r,
            device_id=plan.device(plan.shifted(here, axis, by)),
            device_id_type=MESH,
        )
        copy.start()
        return copy

    def wide(value):
        return value.astype(jnp.float32)

    steps = [k for k in (2, 1, 3) if k < nz] + [0]
    if nz != 4:
        steps = list(range(1, nz)) + [0]
    over_c, over_x, over_z = {}, {}, {}
    for k in steps:
        to = lax.rem(z + k, nz)
        for l in range(1, nc):
            other = lax.rem(c + l, nc)
            for i in range(nx):
                over_c[k, i, l] = send(
                    p_ref.at[to, i, other],
                    got_c.at[k, i, l - 1],
                    "c",
                    l,
                    s_c.at[k, i, l],
                    r_c.at[k, i, l],
                )

    def fold_c(k):
        to = lax.rem(z + k, nz)
        for i in range(nx):
            total = wide(p_ref[to, i, c])
            for l in range(1, nc):
                over_c[k, i, l].wait_recv()
                total += wide(got_c[k, i, l - 1])
            sum_c[k, i] = total.astype(jnp.bfloat16)
        for j in range(1, nx):
            over_x[k, j] = send(
                sum_c.at[k, lax.rem(x + j, nx)],
                got_x.at[k, j - 1],
                "x",
                j,
                s_x.at[k, j],
                r_x.at[k, j],
            )

    def fold_x(k):
        total = wide(sum_c[k, x])
        for j in range(1, nx):
            over_x[k, j].wait_recv()
            total += wide(got_x[k, j - 1])
        if k:
            sum_x[k - 1] = total.astype(jnp.bfloat16)
            over_z[k] = send(sum_x.at[k - 1], got_z.at[k - 1], "z", k, s_z.at[k], r_z.at[k])
            return None
        return total

    for k in steps:
        fold_c(k)
    for k in steps:
        total = fold_x(k)
    for k in steps:
        if k:
            over_z[k].wait_recv()
            total += wide(got_z[k - 1])
    o_ref[...] = (m_ref[...] + total).astype(jnp.bfloat16)
    for copy in [*over_c.values(), *over_x.values(), *over_z.values()]:
        copy.wait_send()


def reduce_add(plan, partial, mid, ident):
    nz, nx, nc = plan.z, plan.x, plan.c
    rows, width = mid.shape
    dma = pltpu.SemaphoreType.DMA

    def buf(*lead):
        return pltpu.VMEM(lead + (rows, width), jnp.bfloat16)

    vmem = pl.BlockSpec(memory_space=pltpu.VMEM)
    return pl.pallas_call(
        functools.partial(reduce_body, plan),
        out_shape=jax.ShapeDtypeStruct(mid.shape, jnp.bfloat16),
        in_specs=[vmem, vmem],
        out_specs=vmem,
        scratch_shapes=[
            buf(nz, nx, max(nc - 1, 1)),
            buf(nz, nx),
            buf(nz, max(nx - 1, 1)),
            buf(max(nz - 1, 1)),
            buf(max(nz - 1, 1)),
            dma((nz, nx, nc)),
            dma((nz, nx, nc)),
            dma((nz, nx)),
            dma((nz, nx)),
            dma((nz,)),
            dma((nz,)),
        ],
        compiler_params=pltpu.CompilerParams(
            collective_id=ident, has_side_effects=True, vmem_limit_bytes=48 * 1024 * 1024
        ),
    )(partial.reshape(nz, nx, nc, rows, width), mid)


def spread(plan, pieces):
    nz, nr = plan.z, plan.r
    z = lax.axis_index("sp") // nr
    r = lax.rem(lax.axis_index("sp"), nr)
    out = jnp.zeros((nz, nr) + pieces.shape[1:], pieces.dtype)
    for k in range(nz):
        block = lax.dynamic_index_in_dim(pieces, lax.rem(z + k, nz), 0, keepdims=False)
        if k:
            block = lax.ppermute(
                block,
                "sp",
                [
                    (a * nr + b, ((a + k) % nz) * nr + b)
                    for a in range(nz)
                    for b in range(nr)
                ],
            )
        source = lax.rem(z + nz - k, nz)
        for j in range(nr):
            given = block
            if j:
                given = lax.ppermute(
                    block,
                    "sp",
                    [
                        (a * nr + b, a * nr + (b + j) % nr)
                        for a in range(nz)
                        for b in range(nr)
                    ],
                )
            at = (source, lax.rem(r + nr - j, nr)) + (0,) * (pieces.ndim - 1)
            out = lax.dynamic_update_slice(out, given[None, None], at)
    return out.reshape((nz * nr,) + pieces.shape[1:])


def shards(
    plan,
    resid_in,
    query_latent,
    kv_latent,
    rotary_key,
    query_gain,
    kv_gain,
    w_query_plain,
    w_query_rotary,
    w_key_plain,
    w_value,
    w_output,
    ffn_gain,
    w_gate,
    w_up,
    w_down,
):
    tok, width = resid_in.shape
    heads_dev = w_query_plain.shape[1] // NOPE
    nz = plan.z
    depth, hidden_dev = w_gate.shape
    part = hidden_dev // nz

    both = jnp.concatenate(
        [w.reshape(depth, nz, part).transpose(1, 0, 2) for w in (w_gate, w_up)], axis=2
    )
    both = spread(plan, both).reshape(-1, 2 * part)
    down = spread(plan, w_down.reshape(nz, part, w_down.shape[1]))

    offset = lax.axis_index("sp") * tok
    position = (offset + jnp.arange(tok, dtype=jnp.int32)).astype(jnp.float32)
    freq = 10000.0 ** (-jnp.arange(0, ROPE, 2, dtype=jnp.float32) / ROPE)
    angle = position[:, None] * freq[None, :]
    cosine = jnp.cos(angle)
    sine = jnp.sin(angle)
    kv_norm = normed(kv_latent, kv_gain).astype(jnp.bfloat16)
    key_rot = rotate(rotary_key.astype(jnp.float32), cosine, sine).astype(jnp.bfloat16)
    piece = tok // plan.c
    packed = lax.dynamic_slice_in_dim(
        jnp.concatenate([kv_norm, key_rot], axis=1),
        lax.rem(lax.axis_index("tp"), plan.c) * piece,
        piece,
        0,
    )
    packed = gather(plan, packed, ("z", "r", "c"), ("z", "r", "c"), 1)
    latent = packed[:, : kv_norm.shape[1]]
    rot_all = packed[:, kv_norm.shape[1] :]
    count = packed.shape[0]

    q_norm = normed(query_latent, query_gain).astype(jnp.bfloat16)
    q_plain = (
        jnp.dot(q_norm, w_query_plain, preferred_element_type=jnp.float32)
        .astype(jnp.bfloat16)
        .reshape(tok, heads_dev, NOPE)
    )
    q_raw = jnp.dot(q_norm, w_query_rotary, preferred_element_type=jnp.float32).reshape(
        tok, heads_dev, ROPE
    )
    q_rot = rotate(q_raw, cosine[:, None, :], sine[:, None, :]).astype(jnp.bfloat16)
    k_all = (
        jnp.dot(latent, w_key_plain, preferred_element_type=jnp.float32)
        .astype(jnp.bfloat16)
        .reshape(count, heads_dev, NOPE)
    )
    v_all = (
        jnp.dot(latent, w_value, preferred_element_type=jnp.float32)
        .astype(jnp.bfloat16)
        .reshape(count, heads_dev, VDIM)
    )
    scale = (NOPE + ROPE) ** (-0.5)
    score = (
        jnp.einsum("qhd,khd->hqk", q_plain, k_all, preferred_element_type=jnp.float32)
        + jnp.einsum("qhr,kr->hqk", q_rot, rot_all, preferred_element_type=jnp.float32)
    ) * scale
    top = jnp.max(score, axis=-1)
    weight = jnp.exp(score - top[:, :, None])
    total = jnp.sum(weight, axis=-1)
    mixed = jnp.einsum(
        "hqk,khd->qhd", weight.astype(jnp.bfloat16), v_all, preferred_element_type=jnp.float32
    )
    attn = (
        (mixed / jnp.transpose(total)[:, :, None])
        .astype(jnp.bfloat16)
        .reshape(tok, heads_dev * VDIM)
    )
    share = tok // plan.tp
    own_start = lax.axis_index("tp") * share
    partial_out = jnp.dot(attn, w_output, preferred_element_type=jnp.float32).astype(jnp.bfloat16)
    terms = swap(plan, partial_out.reshape(plan.tp, share, width), 2)
    mid = lax.dynamic_slice_in_dim(resid_in, own_start, share, 0).astype(jnp.float32) + jnp.sum(
        terms.astype(jnp.float32), axis=0
    )
    h_own = normed(mid, ffn_gain).astype(jnp.bfloat16)
    h_norm = gather(plan, h_own, ("z", "x", "c"), ("z", "x", "c"), 3)

    inner = jnp.dot(h_norm, both, preferred_element_type=jnp.float32)
    hidden = (jax.nn.silu(inner[:, :part]) * inner[:, part:]).astype(jnp.bfloat16)
    partial = jnp.concatenate(
        [
            jnp.dot(hidden, down[i], preferred_element_type=jnp.float32).astype(jnp.bfloat16)
            for i in range(down.shape[0])
        ],
        axis=1,
    )
    return reduce_add(plan, partial, mid, 4)


def solution(mesh):
    plan = Plan(mesh.shape["sp"], mesh.shape["tp"])
    return jax.shard_map(
        functools.partial(shards, plan),
        mesh=mesh,
        in_specs=(
            P("sp", None),
            P("sp", None),
            P("sp", None),
            P("sp", None),
            P(),
            P(),
            P(None, "tp"),
            P(None, "tp"),
            P(None, "tp"),
            P(None, "tp"),
            P("tp", None),
            P(),
            P("sp", "tp"),
            P("sp", "tp"),
            P("tp", "sp"),
        ),
        out_specs=P(("sp", "tp"), None),
        check_vma=False,
    )
```

```python
import functools

import jax
import jax.numpy as jnp
from jax import lax
from jax.experimental import pallas as pl
from jax.experimental.pallas import tpu as pltpu
from jax.sharding import PartitionSpec as P

NOPE = 128
ROPE = 64
VDIM = 128
MESH = pl.DeviceIdType.MESH


def normed(values, gain):
    wide = values.astype(jnp.float32)
    return wide * lax.rsqrt(jnp.mean(wide * wide, axis=-1, keepdims=True) + 1e-06) * gain


def rotate(values, cosine, sine):
    half = values.shape[-1] // 2
    first = values[..., :half]
    second = values[..., half:]
    return jnp.concatenate(
        [first * cosine - second * sine, second * cosine + first * sine], axis=-1
    )


class Plan:
    def __init__(self, sp, tp):
        self.sp, self.tp = sp, tp
        self.z = 4 if sp % 4 == 0 else 1
        self.r = sp // self.z
        self.c = 2 if tp % 2 == 0 else 1
        self.x = tp // self.c

    def sizes(self):
        return {"z": self.z, "r": self.r, "x": self.x, "c": self.c}

    def here(self):
        s, t = lax.axis_index("sp"), lax.axis_index("tp")
        return {"z": s // self.r, "r": lax.rem(s, self.r), "x": t // self.c, "c": lax.rem(t, self.c)}

    def device(self, at):
        return {"sp": at["z"] * self.r + at["r"], "tp": at["x"] * self.c + at["c"]}

    def shifted(self, at, axis, by):
        size = self.sizes()[axis]
        return {**at, axis: lax.rem(at[axis] + (by % size), size)}


def meet(plan, here, axes):
    barrier = pltpu.get_barrier_semaphore()
    count = 0
    for axis in axes:
        for k in range(1, plan.sizes()[axis]):
            pl.semaphore_signal(
                barrier,
                inc=1,
                device_id=plan.device(plan.shifted(here, axis, k)),
                device_id_type=MESH,
            )
            count += 1
    if count:
        pl.semaphore_wait(barrier, count)


def front_body(
    plan,
    heads,
    part,
    kv_ref,
    qp_ref,
    qr_ref,
    wk_ref,
    wv_ref,
    wo_ref,
    resid_ref,
    gain_ref,
    gate_ref,
    up_ref,
    down_ref,
    mid_ref,
    hn_ref,
    both_ref,
    downs_ref,
    packed,
    attn,
    out,
    terms,
    h_own,
    kv_sa,
    kv_ra,
    kv_sb,
    kv_rb,
    kv_sc,
    kv_rc,
    hn_sa,
    hn_ra,
    hn_sb,
    hn_rb,
    hn_sc,
    hn_rc,
    w_sa,
    w_ra,
    w_sb,
    w_rb,
    t_s,
    t_r,
    local,
):
    here = plan.here()
    sizes = plan.sizes()
    nz, nr, tp = plan.z, plan.r, plan.tp
    latent = wk_ref.shape[0]
    depth, full = gate_ref.shape
    narrow = down_ref.shape[1]
    sp_here, tp_here = lax.axis_index("sp"), lax.axis_index("tp")

    barrier = pltpu.get_barrier_semaphore()
    peers = [plan.shifted(here, "z", k) for k in range(1, nz)]
    peers += [plan.shifted(here, "r", k) for k in range(1, nr)]
    peers = [plan.device(at) for at in peers]
    peers += [{"sp": sp_here, "tp": lax.rem(tp_here + k, tp)} for k in range(1, tp)]
    for peer in peers:
        pl.semaphore_signal(barrier, inc=1, device_id=peer, device_id_type=MESH)
    pl.semaphore_wait(barrier, len(peers))

    def send(src, dst, device, sem_s, sem_r):
        copy = pltpu.make_async_remote_copy(
            src_ref=src,
            dst_ref=dst,
            send_sem=sem_s,
            recv_sem=sem_r,
            device_id=device,
            device_id_type=MESH,
        )
        copy.start()
        return copy

    class Gather:
        def __init__(self, axes, x_ref, o_ref, sems, own):
            self.axes, self.x_ref, self.o_ref, self.sems = axes, x_ref, o_ref, sems
            self.copies = {}
            self.mine = pltpu.make_async_copy(x_ref, o_ref.at[self.slot(here)], own)

        def slot(self, at):
            index = 0
            for axis in self.axes:
                index = index * sizes[axis] + at[axis]
            return index

        def send(self, stage, block, by, key):
            mine = len(key) == 0 or not any(key)
            src = self.x_ref if mine else self.o_ref.at[self.slot(block)]
            sem_s, sem_r = self.sems[2 * stage], self.sems[2 * stage + 1]
            at = (key + (by,)) if stage else by
            self.copies[key + (by,)] = send(
                src,
                self.o_ref.at[self.slot(block)],
                plan.device(plan.shifted(here, self.axes[stage], by)),
                sem_s.at[at],
                sem_r.at[at],
            )

        def start(self):
            self.mine.start()
            for k in range(1, sizes[self.axes[0]]):
                self.send(0, here, k, ())

        def run(self):
            na, nb, nc = (sizes[axis] for axis in self.axes)
            for k in range(na):
                block = plan.shifted(here, self.axes[0], -k)
                if k:
                    self.copies[(k,)].wait_recv()
                for j in range(1, nb):
                    self.send(1, block, j, (k,))
                for l in range(1, nc):
                    self.send(2, block, l, (k, 0))
            for k in range(na):
                for j in range(1, nb):
                    self.copies[(k, j)].wait_recv()
                    block = plan.shifted(here, self.axes[0], -k)
                    block = plan.shifted(block, self.axes[1], -j)
                    for l in range(1, nc):
                        self.send(2, block, l, (k, j))

        def finish(self):
            for key, copy in self.copies.items():
                if len(key) == 3:
                    copy.wait_recv()
            for copy in self.copies.values():
                copy.wait_send()
            self.mine.wait()

    def window(index):
        return pl.multiple_of(jnp.minimum(index * part, full - part), 128)

    def targets(sp):
        rows = pl.ds(pl.multiple_of(sp * depth, depth), depth)
        if len(downs_ref.shape) == 3:
            downs = downs_ref.at[sp]
        else:
            downs = downs_ref.at[:, pl.ds(pl.multiple_of(sp * narrow, 128), narrow)]
        return [
            both_ref.at[rows, pl.ds(0, part)],
            both_ref.at[rows, pl.ds(part, part)],
            downs,
        ]

    def sources(index):
        lanes = pl.ds(window(index), part)
        return [gate_ref.at[:, lanes], up_ref.at[:, lanes], down_ref.at[lanes, :]]

    kv = Gather(("z", "r", "c"), kv_ref, packed, (kv_sa, kv_ra, kv_sb, kv_rb, kv_sc, kv_rc), local.at[0])
    kv.start()
    over_z, over_r = {}, {}
    mine = []
    for w in range(3):
        src, dst = sources(here["z"])[w], targets(sp_here)[w]
        mine.append(pltpu.make_async_copy(src, dst, local.at[2 + w]))
        mine[-1].start()
        for k in range(1, nz):
            to = plan.shifted(here, "z", k)
            over_z[w, k] = send(
                sources(to["z"])[w], dst, plan.device(to), w_sa.at[w, k], w_ra.at[w, k]
            )
    kv.run()

    def forward(w, k):
        block = plan.shifted(here, "z", -k)
        dst = targets(block["z"] * nr + here["r"])[w]
        src = dst if k else sources(here["z"])[w]
        if k:
            over_z[w, k].wait_recv()
        for j in range(1, nr):
            over_r[w, k, j] = send(
                src,
                dst,
                plan.device(plan.shifted(here, "r", j)),
                w_sb.at[w, k, j],
                w_rb.at[w, k, j],
            )

    for w in range(3):
        forward(w, 0)
    kv.finish()

    scale = (NOPE + ROPE) ** (-0.5)
    count = packed.shape[0] * packed.shape[1]

    def transposed(left, right):
        return lax.dot_general(
            left, right, (((1,), (1,)), ((), ())), preferred_element_type=jnp.float32
        )

    @pl.loop(0, heads)
    def _(h):
        lanes = pl.ds(pl.multiple_of(h * NOPE, NOPE), NOPE)
        lat = packed[:, :, :latent].reshape(count, latent)
        rot = packed[:, :, latent:].reshape(count, ROPE)
        keys = jnp.dot(lat, wk_ref[:, lanes], preferred_element_type=jnp.float32)
        vals = jnp.dot(lat, wv_ref[:, lanes], preferred_element_type=jnp.float32)
        keys, vals = keys.astype(jnp.bfloat16), vals.astype(jnp.bfloat16)
        score = (transposed(qp_ref[:, lanes], keys) + transposed(qr_ref[h], rot)) * scale
        weight = jnp.exp(score - jnp.max(score, axis=-1, keepdims=True))
        total = jnp.sum(weight, axis=-1, keepdims=True)
        mixed = jnp.dot(weight.astype(jnp.bfloat16), vals, preferred_element_type=jnp.float32)
        attn[:, lanes] = (mixed / total).astype(jnp.bfloat16)

    share = out.shape[1]
    swaps = []
    for k in list(range(1, tp)) + [0]:
        to = lax.rem(tp_here + k, tp)
        rows = pl.ds(pl.multiple_of(to * share, share), share)
        out[to] = jnp.dot(
            attn[rows, :], wo_ref[...], preferred_element_type=jnp.float32
        ).astype(jnp.bfloat16)
        if k:
            swaps.append(
                send(out.at[to], terms.at[k], {"sp": sp_here, "tp": to}, t_s.at[k], t_r.at[k])
            )
    for w in range(2):
        for k in range(1, nz):
            forward(w, k)
    mid = resid_ref[...].astype(jnp.float32) + out[tp_here].astype(jnp.float32)
    for k, copy in enumerate(swaps, 1):
        copy.wait_recv()
        mid += terms[k].astype(jnp.float32)
    mid_ref[...] = mid
    h_own[...] = (
        mid * lax.rsqrt(jnp.mean(mid * mid, axis=-1, keepdims=True) + 1e-06) * gain_ref[...]
    ).astype(jnp.bfloat16)
    hn = Gather(("z", "x", "c"), h_own, hn_ref, (hn_sa, hn_ra, hn_sb, hn_rb, hn_sc, hn_rc), local.at[1])
    hn.start()
    for k in range(1, nz):
        forward(2, k)
    hn.run()
    hn.finish()
    for copy in swaps:
        copy.wait_send()
    for copy in over_r.values():
        copy.wait_recv()
    for copy in [*over_z.values(), *over_r.values()]:
        copy.wait_send()
    for copy in mine:
        copy.wait()


def front(plan, heads, part, kv, qp, qr, wk, wv, wo, resid, gain, gate, up, down, ident):
    nz, nr, nx, nc, tp = plan.z, plan.r, plan.x, plan.c, plan.tp
    share, width = resid.shape
    tok = qp.shape[0]
    dma = pltpu.SemaphoreType.DMA
    vmem = pl.BlockSpec(memory_space=pltpu.VMEM)
    hbm = pl.BlockSpec(memory_space=pl.ANY)

    def sems(a, b, c):
        return [dma((a,)), dma((a,)), dma((a, b)), dma((a, b)), dma((a, b, c)), dma((a, b, c))]

    bf = jnp.bfloat16
    narrow = down.shape[1]
    downs = (part, plan.sp * narrow) if narrow % 128 == 0 else (plan.sp, part, narrow)
    return pl.pallas_call(
        functools.partial(front_body, plan, heads, part),
        out_shape=(
            jax.ShapeDtypeStruct((share, width), jnp.float32),
            jax.ShapeDtypeStruct((nz * tp, share, width), bf),
            jax.ShapeDtypeStruct((plan.sp * gate.shape[0], 2 * part), bf),
            jax.ShapeDtypeStruct(downs, bf),
        ),
        in_specs=[vmem] * 11,
        out_specs=(vmem, hbm, hbm, hbm),
        scratch_shapes=[
            pltpu.VMEM((nz * nr * nc,) + kv.shape, bf),
            pltpu.VMEM((tok, heads * VDIM), bf),
            pltpu.VMEM((tp, share, width), bf),
            pltpu.VMEM((tp, share, width), bf),
            pltpu.VMEM((share, width), bf),
            *sems(nz, nr, nc),
            *sems(nz, nx, nc),
            dma((3, nz)),
            dma((3, nz)),
            dma((3, nz, nr)),
            dma((3, nz, nr)),
            dma((tp,)),
            dma((tp,)),
            dma((5,)),
        ],
        compiler_params=pltpu.CompilerParams(
            collective_id=ident, has_side_effects=True, vmem_limit_bytes=56 * 1024 * 1024
        ),
    )(kv, qp, qr, wk, wv, wo, resid, gain, gate, up, down)


def reduce_body(
    plan, p_ref, m_ref, o_ref, got_c, sum_c, got_x, sum_x, got_z, s_c, r_c, s_x, r_x, s_z, r_z
):
    nz, nx, nc = plan.z, plan.x, plan.c
    here = plan.here()
    z, x, c = here["z"], here["x"], here["c"]
    meet(plan, here, ("z", "x", "c"))

    def send(src, dst, axis, by, sem_s, sem_r):
        copy = pltpu.make_async_remote_copy(
            src_ref=src,
            dst_ref=dst,
            send_sem=sem_s,
            recv_sem=sem_r,
            device_id=plan.device(plan.shifted(here, axis, by)),
            device_id_type=MESH,
        )
        copy.start()
        return copy

    def wide(value):
        return value.astype(jnp.float32)

    steps = [k for k in (2, 1, 3) if k < nz] + [0]
    if nz != 4:
        steps = list(range(1, nz)) + [0]
    over_c, over_x, over_z = {}, {}, {}
    for k in steps:
        to = lax.rem(z + k, nz)
        for l in range(1, nc):
            other = lax.rem(c + l, nc)
            for i in range(nx):
                over_c[k, i, l] = send(
                    p_ref.at[to, i, other],
                    got_c.at[k, i, l - 1],
                    "c",
                    l,
                    s_c.at[k, i, l],
                    r_c.at[k, i, l],
                )

    def fold_c(k):
        to = lax.rem(z + k, nz)
        for i in range(nx):
            total = wide(p_ref[to, i, c])
            for l in range(1, nc):
                over_c[k, i, l].wait_recv()
                total += wide(got_c[k, i, l - 1])
            sum_c[k, i] = total.astype(jnp.bfloat16)
        for j in range(1, nx):
            over_x[k, j] = send(
                sum_c.at[k, lax.rem(x + j, nx)],
                got_x.at[k, j - 1],
                "x",
                j,
                s_x.at[k, j],
                r_x.at[k, j],
            )

    def fold_x(k):
        total = wide(sum_c[k, x])
        for j in range(1, nx):
            over_x[k, j].wait_recv()
            total += wide(got_x[k, j - 1])
        if k:
            sum_x[k - 1] = total.astype(jnp.bfloat16)
            over_z[k] = send(sum_x.at[k - 1], got_z.at[k - 1], "z", k, s_z.at[k], r_z.at[k])
            return None
        return total

    for k in steps:
        fold_c(k)
    for k in steps:
        total = fold_x(k)
    for k in steps:
        if k:
            over_z[k].wait_recv()
            total += wide(got_z[k - 1])
    o_ref[...] = (m_ref[...] + total).astype(jnp.bfloat16)
    for copy in [*over_c.values(), *over_x.values(), *over_z.values()]:
        copy.wait_send()


def reduce_add(plan, partial, mid, ident):
    nz, nx, nc = plan.z, plan.x, plan.c
    rows, width = mid.shape
    dma = pltpu.SemaphoreType.DMA

    def buf(*lead):
        return pltpu.VMEM(lead + (rows, width), jnp.bfloat16)

    vmem = pl.BlockSpec(memory_space=pltpu.VMEM)
    return pl.pallas_call(
        functools.partial(reduce_body, plan),
        out_shape=jax.ShapeDtypeStruct(mid.shape, jnp.bfloat16),
        in_specs=[vmem, vmem],
        out_specs=vmem,
        scratch_shapes=[
            buf(nz, nx, max(nc - 1, 1)),
            buf(nz, nx),
            buf(nz, max(nx - 1, 1)),
            buf(max(nz - 1, 1)),
            buf(max(nz - 1, 1)),
            dma((nz, nx, nc)),
            dma((nz, nx, nc)),
            dma((nz, nx)),
            dma((nz, nx)),
            dma((nz,)),
            dma((nz,)),
        ],
        compiler_params=pltpu.CompilerParams(
            collective_id=ident, has_side_effects=True, vmem_limit_bytes=48 * 1024 * 1024
        ),
    )(partial.reshape(nz, nx, nc, rows, width), mid)


def shards(
    plan,
    resid_in,
    query_latent,
    kv_latent,
    rotary_key,
    query_gain,
    kv_gain,
    w_query_plain,
    w_query_rotary,
    w_key_plain,
    w_value,
    w_output,
    ffn_gain,
    w_gate,
    w_up,
    w_down,
):
    tok, width = resid_in.shape
    heads_dev = w_query_plain.shape[1] // NOPE
    nz = plan.z
    hidden_dev = w_gate.shape[1]
    part = min(-(-hidden_dev // (nz * 128)) * 128, hidden_dev)

    offset = lax.axis_index("sp") * tok
    position = (offset + jnp.arange(tok, dtype=jnp.int32)).astype(jnp.float32)
    freq = 10000.0 ** (-jnp.arange(0, ROPE, 2, dtype=jnp.float32) / ROPE)
    angle = position[:, None] * freq[None, :]
    cosine = jnp.cos(angle)
    sine = jnp.sin(angle)
    kv_norm = normed(kv_latent, kv_gain).astype(jnp.bfloat16)
    key_rot = rotate(rotary_key.astype(jnp.float32), cosine, sine).astype(jnp.bfloat16)
    piece = tok // plan.c
    packed = lax.dynamic_slice_in_dim(
        jnp.concatenate([kv_norm, key_rot], axis=1),
        lax.rem(lax.axis_index("tp"), plan.c) * piece,
        piece,
        0,
    )
    q_norm = normed(query_latent, query_gain).astype(jnp.bfloat16)
    q_plain = (
        jnp.dot(q_norm, w_query_plain, preferred_element_type=jnp.float32)
        .astype(jnp.bfloat16)
    )
    q_raw = jnp.dot(q_norm, w_query_rotary, preferred_element_type=jnp.float32).reshape(
        tok, heads_dev, ROPE
    )
    q_rot = rotate(q_raw, cosine[:, None, :], sine[:, None, :]).astype(jnp.bfloat16)
    share = tok // plan.tp
    own_start = lax.axis_index("tp") * share
    mid, h_norm, both, down = front(
        plan,
        heads_dev,
        part,
        packed,
        q_plain,
        jnp.transpose(q_rot, (1, 0, 2)),
        w_key_plain,
        w_value,
        w_output,
        lax.dynamic_slice_in_dim(resid_in, own_start, share, 0),
        ffn_gain[None, :],
        w_gate,
        w_up,
        w_down,
        1,
    )
    if down.ndim == 3:
        down = jnp.transpose(down, (1, 0, 2)).reshape(part, width)
    inner = jnp.dot(h_norm.reshape(-1, width), both, preferred_element_type=jnp.float32)
    place = lax.axis_index("sp") // plan.r * part
    lane = lax.broadcasted_iota(jnp.int32, (1, part), 1)
    fresh = lane >= place - jnp.minimum(place, hidden_dev - part)
    hidden = jnp.where(fresh, jax.nn.silu(inner[:, :part]) * inner[:, part:], 0.0)
    partial = jnp.dot(hidden.astype(jnp.bfloat16), down, preferred_element_type=jnp.float32)
    return reduce_add(plan, partial.astype(jnp.bfloat16), mid, 2)


def solution(mesh):
    plan = Plan(mesh.shape["sp"], mesh.shape["tp"])
    return jax.shard_map(
        functools.partial(shards, plan),
        mesh=mesh,
        in_specs=(
            P("sp", None),
            P("sp", None),
            P("sp", None),
            P("sp", None),
            P(),
            P(),
            P(None, "tp"),
            P(None, "tp"),
            P(None, "tp"),
            P(None, "tp"),
            P("tp", None),
            P(),
            P("sp", "tp"),
            P("sp", "tp"),
            P("tp", "sp"),
        ),
        out_specs=P(("sp", "tp"), None),
        check_vma=False,
    )
```

```python
import functools

import jax
import jax.numpy as jnp
from jax import lax
from jax.experimental import pallas as pl
from jax.experimental.pallas import tpu as pltpu
from jax.sharding import PartitionSpec as P

NOPE = 128
ROPE = 64
VDIM = 128
MESH = pl.DeviceIdType.MESH


def normed(values, gain):
    wide = values.astype(jnp.float32)
    return wide * lax.rsqrt(jnp.mean(wide * wide, axis=-1, keepdims=True) + 1e-06) * gain


def rotate(values, cosine, sine):
    half = values.shape[-1] // 2
    first = values[..., :half]
    second = values[..., half:]
    return jnp.concatenate(
        [first * cosine - second * sine, second * cosine + first * sine], axis=-1
    )


class Plan:
    def __init__(self, sp, tp):
        self.sp, self.tp = sp, tp
        self.z = 4 if sp % 4 == 0 else 1
        self.r = sp // self.z
        self.c = 2 if tp % 2 == 0 else 1
        self.x = tp // self.c

    def sizes(self):
        return {"z": self.z, "r": self.r, "x": self.x, "c": self.c}

    def here(self):
        s, t = lax.axis_index("sp"), lax.axis_index("tp")
        return {"z": s // self.r, "r": lax.rem(s, self.r), "x": t // self.c, "c": lax.rem(t, self.c)}

    def device(self, at):
        return {"sp": at["z"] * self.r + at["r"], "tp": at["x"] * self.c + at["c"]}

    def shifted(self, at, axis, by):
        size = self.sizes()[axis]
        return {**at, axis: lax.rem(at[axis] + (by % size), size)}


def front_body(
    plan,
    heads,
    part,
    kv_ref,
    qp_ref,
    qr_ref,
    wk_ref,
    wv_ref,
    wo_ref,
    resid_ref,
    gain_ref,
    gate_ref,
    up_ref,
    down_ref,
    o_ref,
    mid_ref,
    hn_ref,
    both_ref,
    downs_ref,
    packed,
    attn,
    out,
    terms,
    h_own,
    part_ref,
    got_c,
    sum_c,
    got_x,
    sum_x,
    got_z,
    kv_sa,
    kv_ra,
    kv_sb,
    kv_rb,
    kv_sc,
    kv_rc,
    hn_sa,
    hn_ra,
    hn_sb,
    hn_rb,
    hn_sc,
    hn_rc,
    w_sa,
    w_ra,
    w_sb,
    w_rb,
    t_s,
    t_r,
    c_s,
    c_r,
    x_s,
    x_r,
    z_s,
    z_r,
    local,
):
    here = plan.here()
    sizes = plan.sizes()
    nz, nr, tp = plan.z, plan.r, plan.tp
    latent = wk_ref.shape[0]
    depth, full = gate_ref.shape
    narrow = down_ref.shape[1]
    sp_here, tp_here = lax.axis_index("sp"), lax.axis_index("tp")

    barrier = pltpu.get_barrier_semaphore()
    peers = [plan.shifted(here, "z", k) for k in range(1, nz)]
    peers += [plan.shifted(here, "r", k) for k in range(1, nr)]
    peers = [plan.device(at) for at in peers]
    peers += [{"sp": sp_here, "tp": lax.rem(tp_here + k, tp)} for k in range(1, tp)]
    for peer in peers:
        pl.semaphore_signal(barrier, inc=1, device_id=peer, device_id_type=MESH)
    pl.semaphore_wait(barrier, len(peers))

    def send(src, dst, device, sem_s, sem_r):
        copy = pltpu.make_async_remote_copy(
            src_ref=src,
            dst_ref=dst,
            send_sem=sem_s,
            recv_sem=sem_r,
            device_id=device,
            device_id_type=MESH,
        )
        copy.start()
        return copy

    class Gather:
        def __init__(self, axes, x_ref, o_ref, sems, own):
            self.axes, self.x_ref, self.o_ref, self.sems = axes, x_ref, o_ref, sems
            self.copies = {}
            self.mine = pltpu.make_async_copy(x_ref, o_ref.at[self.slot(here)], own)

        def slot(self, at):
            index = 0
            for axis in self.axes:
                index = index * sizes[axis] + at[axis]
            return index

        def send(self, stage, block, by, key):
            mine = len(key) == 0 or not any(key)
            src = self.x_ref if mine else self.o_ref.at[self.slot(block)]
            sem_s, sem_r = self.sems[2 * stage], self.sems[2 * stage + 1]
            at = (key + (by,)) if stage else by
            self.copies[key + (by,)] = send(
                src,
                self.o_ref.at[self.slot(block)],
                plan.device(plan.shifted(here, self.axes[stage], by)),
                sem_s.at[at],
                sem_r.at[at],
            )

        def start(self):
            self.mine.start()
            for k in range(1, sizes[self.axes[0]]):
                self.send(0, here, k, ())

        def relay(self, k):
            block = plan.shifted(here, self.axes[0], -k)
            if k:
                self.copies[(k,)].wait_recv()
            for j in range(1, sizes[self.axes[1]]):
                self.send(1, block, j, (k,))
            for l in range(1, sizes[self.axes[2]]):
                self.send(2, block, l, (k, 0))

        def relay_on(self, k):
            for j in range(1, sizes[self.axes[1]]):
                self.copies[(k, j)].wait_recv()
                block = plan.shifted(here, self.axes[0], -k)
                block = plan.shifted(block, self.axes[1], -j)
                for l in range(1, sizes[self.axes[2]]):
                    self.send(2, block, l, (k, j))

        def landed(self, k):
            if k == 0:
                self.mine.wait()
            for key, copy in self.copies.items():
                if len(key) == 3 and key[0] == k:
                    copy.wait_recv()

        def finish(self):
            for copy in self.copies.values():
                copy.wait_send()

    def window(index):
        return pl.multiple_of(jnp.minimum(index * part, full - part), 128)

    def targets(sp):
        rows = pl.ds(pl.multiple_of(sp * depth, depth), depth)
        if len(downs_ref.shape) == 3:
            downs = downs_ref.at[sp]
        else:
            downs = downs_ref.at[:, pl.ds(pl.multiple_of(sp * narrow, 128), narrow)]
        return [
            both_ref.at[rows, pl.ds(0, part)],
            both_ref.at[rows, pl.ds(part, part)],
            downs,
        ]

    def sources(index):
        lanes = pl.ds(window(index), part)
        return [gate_ref.at[:, lanes], up_ref.at[:, lanes], down_ref.at[lanes, :]]

    kv = Gather(("z", "r", "c"), kv_ref, packed, (kv_sa, kv_ra, kv_sb, kv_rb, kv_sc, kv_rc), local.at[0])
    kv.start()
    over_z, over_r = {}, {}
    mine = []
    for w in range(3):
        src, dst = sources(here["z"])[w], targets(sp_here)[w]
        mine.append(pltpu.make_async_copy(src, dst, local.at[2 + w]))
        mine[-1].start()
        for k in range(1, nz):
            to = plan.shifted(here, "z", k)
            over_z[w, k] = send(
                sources(to["z"])[w], dst, plan.device(to), w_sa.at[w, k], w_ra.at[w, k]
            )
    for k in range(nz):
        kv.relay(k)
    for k in range(nz):
        kv.relay_on(k)

    def forward(w, k):
        block = plan.shifted(here, "z", -k)
        dst = targets(block["z"] * nr + here["r"])[w]
        src = dst if k else sources(here["z"])[w]
        if k:
            over_z[w, k].wait_recv()
        for j in range(1, nr):
            over_r[w, k, j] = send(
                src,
                dst,
                plan.device(plan.shifted(here, "r", j)),
                w_sb.at[w, k, j],
                w_rb.at[w, k, j],
            )

    for w in range(3):
        forward(w, 0)
    for k in range(nz):
        kv.landed(k)

    scale = (NOPE + ROPE) ** (-0.5)
    count = packed.shape[0] * packed.shape[1]

    def transposed(left, right):
        return lax.dot_general(
            left, right, (((1,), (1,)), ((), ())), preferred_element_type=jnp.float32
        )

    @pl.loop(0, heads)
    def _(h):
        lanes = pl.ds(pl.multiple_of(h * NOPE, NOPE), NOPE)
        lat = packed[:, :, :latent].reshape(count, latent)
        rot = packed[:, :, latent:].reshape(count, ROPE)
        keys = jnp.dot(lat, wk_ref[:, lanes], preferred_element_type=jnp.float32)
        vals = jnp.dot(lat, wv_ref[:, lanes], preferred_element_type=jnp.float32)
        keys, vals = keys.astype(jnp.bfloat16), vals.astype(jnp.bfloat16)
        score = (transposed(qp_ref[:, lanes], keys) + transposed(qr_ref[h], rot)) * scale
        weight = jnp.exp(score - jnp.max(score, axis=-1, keepdims=True))
        total = jnp.sum(weight, axis=-1, keepdims=True)
        mixed = jnp.dot(weight.astype(jnp.bfloat16), vals, preferred_element_type=jnp.float32)
        attn[:, lanes] = (mixed / total).astype(jnp.bfloat16)

    share = out.shape[1]
    swaps = []
    for k in list(range(1, tp)) + [0]:
        to = lax.rem(tp_here + k, tp)
        rows = pl.ds(pl.multiple_of(to * share, share), share)
        out[to] = jnp.dot(
            attn[rows, :], wo_ref[...], preferred_element_type=jnp.float32
        ).astype(jnp.bfloat16)
        if k:
            swaps.append(
                send(out.at[to], terms.at[k], {"sp": sp_here, "tp": to}, t_s.at[k], t_r.at[k])
            )
    for w in range(2):
        for k in range(1, nz):
            forward(w, k)
    mid = resid_ref[...].astype(jnp.float32) + out[tp_here].astype(jnp.float32)
    for k, copy in enumerate(swaps, 1):
        copy.wait_recv()
        mid += terms[k].astype(jnp.float32)
    mid_ref[...] = mid
    h_own[...] = (
        mid * lax.rsqrt(jnp.mean(mid * mid, axis=-1, keepdims=True) + 1e-06) * gain_ref[...]
    ).astype(jnp.bfloat16)
    hn = Gather(("z", "x", "c"), h_own, hn_ref, (hn_sa, hn_ra, hn_sb, hn_rb, hn_sc, hn_rc), local.at[1])
    hn.start()
    hn.relay(0)
    for k in range(1, nz):
        forward(2, k)
    for copy in over_r.values():
        copy.wait_recv()
    for copy in mine:
        copy.wait()

    nx, nc = plan.x, plan.c
    x, c = here["x"], here["c"]
    place = here["z"] * part
    lane = lax.broadcasted_iota(jnp.int32, (1, part), 1)
    fresh = lane >= place - jnp.minimum(place, full - part)
    wide = jnp.float32
    over_c, over_x, back = {}, {}, {}

    def feed(k):
        first = plan.shifted(here, "z", -k)["z"] * tp
        rows = hn_ref[pl.ds(first, tp)].reshape(tp * share, -1)
        inner = jnp.dot(rows, both_ref[...], preferred_element_type=wide)
        hidden = jnp.where(fresh, jax.nn.silu(inner[:, :part]) * inner[:, part:], 0.0)
        hidden = hidden.astype(jnp.bfloat16)
        if len(downs_ref.shape) == 3:
            for i in range(downs_ref.shape[0]):
                piece = jnp.dot(hidden, downs_ref[i], preferred_element_type=wide)
                part_ref[k, :, :, :, i * narrow : (i + 1) * narrow] = piece.astype(
                    jnp.bfloat16
                ).reshape(nx, nc, share, narrow)
        else:
            piece = jnp.dot(hidden, downs_ref[...], preferred_element_type=wide)
            part_ref[k] = piece.astype(jnp.bfloat16).reshape(nx, nc, share, -1)
        for l in range(1, nc):
            for i in range(nx):
                over_c[k, i, l] = send(
                    part_ref.at[k, i, lax.rem(c + l, nc)],
                    got_c.at[k, i, l - 1],
                    plan.device(plan.shifted(here, "c", l)),
                    c_s.at[k, i, l],
                    c_r.at[k, i, l],
                )

    def fold_c(k):
        for i in range(nx):
            total = part_ref[k, i, c].astype(wide)
            for l in range(1, nc):
                over_c[k, i, l].wait_recv()
                total += got_c[k, i, l - 1].astype(wide)
            sum_c[k, i] = total.astype(jnp.bfloat16)
        for j in range(1, nx):
            over_x[k, j] = send(
                sum_c.at[k, lax.rem(x + j, nx)],
                got_x.at[k, j - 1],
                plan.device(plan.shifted(here, "x", j)),
                x_s.at[k, j],
                x_r.at[k, j],
            )

    def fold_x(k):
        total = sum_c[k, x].astype(wide)
        for j in range(1, nx):
            over_x[k, j].wait_recv()
            total += got_x[k, j - 1].astype(wide)
        if k == 0:
            mid_ref[...] += total
            return
        sum_x[k - 1] = total.astype(jnp.bfloat16)
        back[k] = send(
            sum_x.at[k - 1],
            got_z.at[k - 1],
            plan.device(plan.shifted(here, "z", -k)),
            z_s.at[k],
            z_r.at[k],
        )

    for k in range(nz):
        if k + 1 < nz:
            hn.relay(k + 1)
        hn.relay_on(k)
        hn.landed(k)
        feed(k)
        if k:
            fold_x(k - 1)
        fold_c(k)
    fold_x(nz - 1)
    total = mid_ref[...]
    for k in range(1, nz):
        back[k].wait_recv()
        total += got_z[k - 1].astype(wide)
    o_ref[...] = total.astype(jnp.bfloat16)
    kv.finish()
    hn.finish()
    for copies in (over_z, over_r, over_c, over_x, back):
        for copy in copies.values():
            copy.wait_send()
    for copy in swaps:
        copy.wait_send()


def front(plan, heads, part, kv, qp, qr, wk, wv, wo, resid, gain, gate, up, down, ident):
    nz, nr, nx, nc, tp = plan.z, plan.r, plan.x, plan.c, plan.tp
    share, width = resid.shape
    tok = qp.shape[0]
    dma = pltpu.SemaphoreType.DMA
    vmem = pl.BlockSpec(memory_space=pltpu.VMEM)

    def sems(a, b, c):
        return [dma((a,)), dma((a,)), dma((a, b)), dma((a, b)), dma((a, b, c)), dma((a, b, c))]

    bf = jnp.bfloat16
    narrow = down.shape[1]
    downs = (part, plan.sp * narrow) if narrow % 128 == 0 else (plan.sp, part, narrow)
    return pl.pallas_call(
        functools.partial(front_body, plan, heads, part),
        out_shape=jax.ShapeDtypeStruct((share, width), bf),
        in_specs=[vmem] * 11,
        out_specs=vmem,
        scratch_shapes=[
            pltpu.VMEM((share, width), jnp.float32),
            pltpu.VMEM((nz * tp, share, width), bf),
            pltpu.VMEM((plan.sp * gate.shape[0], 2 * part), bf),
            pltpu.VMEM(downs, bf),
            pltpu.VMEM((nz * nr * nc,) + kv.shape, bf),
            pltpu.VMEM((tok, heads * VDIM), bf),
            pltpu.VMEM((tp, share, width), bf),
            pltpu.VMEM((tp, share, width), bf),
            pltpu.VMEM((share, width), bf),
            pltpu.VMEM((nz, nx, nc, share, width), bf),
            pltpu.VMEM((nz, nx, max(nc - 1, 1), share, width), bf),
            pltpu.VMEM((nz, nx, share, width), bf),
            pltpu.VMEM((nz, max(nx - 1, 1), share, width), bf),
            pltpu.VMEM((max(nz - 1, 1), share, width), bf),
            pltpu.VMEM((max(nz - 1, 1), share, width), bf),
            *sems(nz, nr, nc),
            *sems(nz, nx, nc),
            dma((3, nz)),
            dma((3, nz)),
            dma((3, nz, nr)),
            dma((3, nz, nr)),
            dma((tp,)),
            dma((tp,)),
            dma((nz, nx, nc)),
            dma((nz, nx, nc)),
            dma((nz, nx)),
            dma((nz, nx)),
            dma((nz,)),
            dma((nz,)),
            dma((5,)),
        ],
        compiler_params=pltpu.CompilerParams(
            collective_id=ident, has_side_effects=True, vmem_limit_bytes=62 * 1024 * 1024
        ),
    )(kv, qp, qr, wk, wv, wo, resid, gain, gate, up, down)


def shards(
    plan,
    resid_in,
    query_latent,
    kv_latent,
    rotary_key,
    query_gain,
    kv_gain,
    w_query_plain,
    w_query_rotary,
    w_key_plain,
    w_value,
    w_output,
    ffn_gain,
    w_gate,
    w_up,
    w_down,
):
    tok = resid_in.shape[0]
    heads_dev = w_query_plain.shape[1] // NOPE
    nz = plan.z
    hidden_dev = w_gate.shape[1]
    part = min(-(-hidden_dev // (nz * 128)) * 128, hidden_dev)

    offset = lax.axis_index("sp") * tok
    position = (offset + jnp.arange(tok, dtype=jnp.int32)).astype(jnp.float32)
    freq = 10000.0 ** (-jnp.arange(0, ROPE, 2, dtype=jnp.float32) / ROPE)
    angle = position[:, None] * freq[None, :]
    cosine = jnp.cos(angle)
    sine = jnp.sin(angle)
    kv_norm = normed(kv_latent, kv_gain).astype(jnp.bfloat16)
    key_rot = rotate(rotary_key.astype(jnp.float32), cosine, sine).astype(jnp.bfloat16)
    piece = tok // plan.c
    packed = lax.dynamic_slice_in_dim(
        jnp.concatenate([kv_norm, key_rot], axis=1),
        lax.rem(lax.axis_index("tp"), plan.c) * piece,
        piece,
        0,
    )
    q_norm = normed(query_latent, query_gain).astype(jnp.bfloat16)
    q_plain = (
        jnp.dot(q_norm, w_query_plain, preferred_element_type=jnp.float32)
        .astype(jnp.bfloat16)
    )
    q_raw = jnp.dot(q_norm, w_query_rotary, preferred_element_type=jnp.float32).reshape(
        tok, heads_dev, ROPE
    )
    q_rot = rotate(q_raw, cosine[:, None, :], sine[:, None, :]).astype(jnp.bfloat16)
    share = tok // plan.tp
    own_start = lax.axis_index("tp") * share
    return front(
        plan,
        heads_dev,
        part,
        packed,
        q_plain,
        jnp.transpose(q_rot, (1, 0, 2)),
        w_key_plain,
        w_value,
        w_output,
        lax.dynamic_slice_in_dim(resid_in, own_start, share, 0),
        ffn_gain[None, :],
        w_gate,
        w_up,
        w_down,
        1,
    )


def solution(mesh):
    plan = Plan(mesh.shape["sp"], mesh.shape["tp"])
    return jax.shard_map(
        functools.partial(shards, plan),
        mesh=mesh,
        in_specs=(
            P("sp", None),
            P("sp", None),
            P("sp", None),
            P("sp", None),
            P(),
            P(),
            P(None, "tp"),
            P(None, "tp"),
            P(None, "tp"),
            P(None, "tp"),
            P("tp", None),
            P(),
            P("sp", "tp"),
            P("sp", "tp"),
            P("tp", "sp"),
        ),
        out_specs=P(("sp", "tp"), None),
        check_vma=False,
    )
```

```python
import functools

import jax
import jax.numpy as jnp
from jax import lax
from jax.experimental import pallas as pl
from jax.experimental.pallas import tpu as pltpu
from jax.sharding import PartitionSpec as P

NOPE = 128
ROPE = 64
VDIM = 128
MESH = pl.DeviceIdType.MESH


def normed(values, gain):
    wide = values.astype(jnp.float32)
    return wide * lax.rsqrt(jnp.mean(wide * wide, axis=-1, keepdims=True) + 1e-06) * gain


def rotate(values, cosine, sine):
    half = values.shape[-1] // 2
    first = values[..., :half]
    second = values[..., half:]
    return jnp.concatenate(
        [first * cosine - second * sine, second * cosine + first * sine], axis=-1
    )


class Plan:
    def __init__(self, sp, tp):
        self.sp, self.tp = sp, tp
        self.z = 4 if sp % 4 == 0 else 1
        self.r = sp // self.z
        self.c = 2 if tp % 2 == 0 else 1
        self.x = tp // self.c

    def sizes(self):
        return {"z": self.z, "r": self.r, "x": self.x, "c": self.c}

    def here(self):
        s, t = lax.axis_index("sp"), lax.axis_index("tp")
        return {"z": s // self.r, "r": lax.rem(s, self.r), "x": t // self.c, "c": lax.rem(t, self.c)}

    def device(self, at):
        return {"sp": at["z"] * self.r + at["r"], "tp": at["x"] * self.c + at["c"]}

    def shifted(self, at, axis, by):
        size = self.sizes()[axis]
        return {**at, axis: lax.rem(at[axis] + (by % size), size)}


def front_body(
    plan,
    heads,
    part,
    kv_ref,
    qp_ref,
    qr_ref,
    wk_ref,
    wv_ref,
    wo_ref,
    resid_ref,
    gain_ref,
    gate_ref,
    up_ref,
    down_ref,
    o_ref,
    mid_ref,
    hn_ref,
    both_ref,
    downs_ref,
    packed,
    attn,
    out,
    terms,
    h_own,
    part_ref,
    got_c,
    sum_c,
    got_x,
    sum_x,
    got_z,
    kv_sa,
    kv_ra,
    kv_sb,
    kv_rb,
    kv_sc,
    kv_rc,
    hn_sa,
    hn_ra,
    hn_sb,
    hn_rb,
    hn_sc,
    hn_rc,
    w_sa,
    w_ra,
    w_sb,
    w_rb,
    t_s,
    t_r,
    c_s,
    c_r,
    x_s,
    x_r,
    z_s,
    z_r,
    local,
):
    here = plan.here()
    sizes = plan.sizes()
    nz, nr, tp = plan.z, plan.r, plan.tp
    latent = wk_ref.shape[0]
    depth, full = gate_ref.shape
    narrow = down_ref.shape[1]
    sp_here, tp_here = lax.axis_index("sp"), lax.axis_index("tp")

    barrier = pltpu.get_barrier_semaphore()
    peers = [plan.shifted(here, "z", k) for k in range(1, nz)]
    peers += [plan.shifted(here, "r", k) for k in range(1, nr)]
    peers = [plan.device(at) for at in peers]
    peers += [{"sp": sp_here, "tp": lax.rem(tp_here + k, tp)} for k in range(1, tp)]
    for peer in peers:
        pl.semaphore_signal(barrier, inc=1, device_id=peer, device_id_type=MESH)
    pl.semaphore_wait(barrier, len(peers))

    def send(src, dst, device, sem_s, sem_r):
        copy = pltpu.make_async_remote_copy(
            src_ref=src,
            dst_ref=dst,
            send_sem=sem_s,
            recv_sem=sem_r,
            device_id=device,
            device_id_type=MESH,
        )
        copy.start()
        return copy

    class Gather:
        def __init__(self, axes, x_ref, o_ref, sems, own):
            self.axes, self.x_ref, self.o_ref, self.sems = axes, x_ref, o_ref, sems
            self.copies = {}
            self.mine = pltpu.make_async_copy(x_ref, o_ref.at[self.slot(here)], own)

        def slot(self, at):
            index = 0
            for axis in self.axes:
                index = index * sizes[axis] + at[axis]
            return index

        def send(self, stage, block, by, key):
            mine = len(key) == 0 or not any(key)
            src = self.x_ref if mine else self.o_ref.at[self.slot(block)]
            sem_s, sem_r = self.sems[2 * stage], self.sems[2 * stage + 1]
            at = (key + (by,)) if stage else by
            self.copies[key + (by,)] = send(
                src,
                self.o_ref.at[self.slot(block)],
                plan.device(plan.shifted(here, self.axes[stage], by)),
                sem_s.at[at],
                sem_r.at[at],
            )

        def start(self):
            self.mine.start()
            for k in range(1, sizes[self.axes[0]]):
                self.send(0, here, k, ())

        def relay(self, k):
            block = plan.shifted(here, self.axes[0], -k)
            if k:
                self.copies[(k,)].wait_recv()
            for j in range(1, sizes[self.axes[1]]):
                self.send(1, block, j, (k,))
            for l in range(1, sizes[self.axes[2]]):
                self.send(2, block, l, (k, 0))

        def relay_on(self, k):
            for j in range(1, sizes[self.axes[1]]):
                self.copies[(k, j)].wait_recv()
                block = plan.shifted(here, self.axes[0], -k)
                block = plan.shifted(block, self.axes[1], -j)
                for l in range(1, sizes[self.axes[2]]):
                    self.send(2, block, l, (k, j))

        def landed(self, k):
            if k == 0:
                self.mine.wait()
            for key, copy in self.copies.items():
                if len(key) == 3 and key[0] == k:
                    copy.wait_recv()

        def finish(self):
            for copy in self.copies.values():
                copy.wait_send()

    def window(index):
        return pl.multiple_of(jnp.minimum(index * part, full - part), 128)

    def targets(sp):
        rows = pl.ds(pl.multiple_of(sp * depth, depth), depth)
        if len(downs_ref.shape) == 3:
            downs = downs_ref.at[sp]
        else:
            downs = downs_ref.at[:, pl.ds(pl.multiple_of(sp * narrow, 128), narrow)]
        return [
            both_ref.at[rows, pl.ds(0, part)],
            both_ref.at[rows, pl.ds(part, part)],
            downs,
        ]

    def sources(index):
        lanes = pl.ds(window(index), part)
        return [gate_ref.at[:, lanes], up_ref.at[:, lanes], down_ref.at[lanes, :]]

    kv = Gather(("z", "r", "c"), kv_ref, packed, (kv_sa, kv_ra, kv_sb, kv_rb, kv_sc, kv_rc), local.at[0])
    kv.start()
    over_z, over_r = {}, {}
    mine = []
    for w in range(3):
        src, dst = sources(here["z"])[w], targets(sp_here)[w]
        mine.append(pltpu.make_async_copy(src, dst, local.at[2 + w]))
        mine[-1].start()
        for k in range(1, nz):
            to = plan.shifted(here, "z", k)
            over_z[w, k] = send(
                sources(to["z"])[w], dst, plan.device(to), w_sa.at[w, k], w_ra.at[w, k]
            )
    for k in range(nz):
        kv.relay(k)
    for k in range(nz):
        kv.relay_on(k)

    def forward(w, k):
        block = plan.shifted(here, "z", -k)
        dst = targets(block["z"] * nr + here["r"])[w]
        src = dst if k else sources(here["z"])[w]
        if k:
            over_z[w, k].wait_recv()
        for j in range(1, nr):
            over_r[w, k, j] = send(
                src,
                dst,
                plan.device(plan.shifted(here, "r", j)),
                w_sb.at[w, k, j],
                w_rb.at[w, k, j],
            )

    for w in range(3):
        forward(w, 0)
    for k in range(nz):
        kv.landed(k)

    scale = (NOPE + ROPE) ** (-0.5)
    count = packed.shape[0] * packed.shape[1]

    def transposed(left, right):
        return lax.dot_general(
            left, right, (((1,), (1,)), ((), ())), preferred_element_type=jnp.float32
        )

    @pl.loop(0, heads)
    def _(h):
        lanes = pl.ds(pl.multiple_of(h * NOPE, NOPE), NOPE)
        lat = packed[:, :, :latent].reshape(count, latent)
        rot = packed[:, :, latent:].reshape(count, ROPE)
        keys = jnp.dot(lat, wk_ref[:, lanes], preferred_element_type=jnp.float32)
        vals = jnp.dot(lat, wv_ref[:, lanes], preferred_element_type=jnp.float32)
        keys, vals = keys.astype(jnp.bfloat16), vals.astype(jnp.bfloat16)
        score = (transposed(qp_ref[:, lanes], keys) + transposed(qr_ref[h], rot)) * scale
        weight = jnp.exp(score - jnp.max(score, axis=-1, keepdims=True))
        total = jnp.sum(weight, axis=-1, keepdims=True)
        mixed = jnp.dot(weight.astype(jnp.bfloat16), vals, preferred_element_type=jnp.float32)
        attn[:, lanes] = (mixed / total).astype(jnp.bfloat16)

    for k in range(1, nz):
        forward(0, k)
    share = out.shape[1]
    swaps = []
    for k in list(range(1, tp)) + [0]:
        to = lax.rem(tp_here + k, tp)
        rows = pl.ds(pl.multiple_of(to * share, share), share)
        out[to] = jnp.dot(
            attn[rows, :], wo_ref[...], preferred_element_type=jnp.float32
        ).astype(jnp.bfloat16)
        if k:
            swaps.append(
                send(out.at[to], terms.at[k], {"sp": sp_here, "tp": to}, t_s.at[k], t_r.at[k])
            )
    for k in range(1, nz):
        forward(1, k)
    mid = resid_ref[...].astype(jnp.float32) + out[tp_here].astype(jnp.float32)
    for k, copy in enumerate(swaps, 1):
        copy.wait_recv()
        mid += terms[k].astype(jnp.float32)
    mid_ref[...] = mid
    h_own[...] = (
        mid * lax.rsqrt(jnp.mean(mid * mid, axis=-1, keepdims=True) + 1e-06) * gain_ref[...]
    ).astype(jnp.bfloat16)
    hn = Gather(("z", "x", "c"), h_own, hn_ref, (hn_sa, hn_ra, hn_sb, hn_rb, hn_sc, hn_rc), local.at[1])
    hn.start()
    hn.relay(0)
    for k in range(1, nz):
        forward(2, k)
    for copy in over_r.values():
        copy.wait_recv()
    for copy in mine:
        copy.wait()

    nx, nc = plan.x, plan.c
    x, c = here["x"], here["c"]
    place = here["z"] * part
    lane = lax.broadcasted_iota(jnp.int32, (1, part), 1)
    fresh = lane >= place - jnp.minimum(place, full - part)
    wide = jnp.float32
    over_c, over_x, back = {}, {}, {}

    def feed(k):
        first = plan.shifted(here, "z", -k)["z"] * tp
        rows = hn_ref[pl.ds(first, tp)].reshape(tp * share, -1)
        inner = jnp.dot(rows, both_ref[...], preferred_element_type=wide)
        hidden = jnp.where(fresh, jax.nn.silu(inner[:, :part]) * inner[:, part:], 0.0)
        hidden = hidden.astype(jnp.bfloat16)
        if len(downs_ref.shape) == 3:
            for i in range(downs_ref.shape[0]):
                piece = jnp.dot(hidden, downs_ref[i], preferred_element_type=wide)
                part_ref[k, :, :, :, i * narrow : (i + 1) * narrow] = piece.astype(
                    jnp.bfloat16
                ).reshape(nx, nc, share, narrow)
        else:
            piece = jnp.dot(hidden, downs_ref[...], preferred_element_type=wide)
            part_ref[k] = piece.astype(jnp.bfloat16).reshape(nx, nc, share, -1)
        for l in range(1, nc):
            for i in range(nx):
                over_c[k, i, l] = send(
                    part_ref.at[k, i, lax.rem(c + l, nc)],
                    got_c.at[k, i, l - 1],
                    plan.device(plan.shifted(here, "c", l)),
                    c_s.at[k, i, l],
                    c_r.at[k, i, l],
                )

    def fold_c(k):
        for i in range(nx):
            total = part_ref[k, i, c].astype(wide)
            for l in range(1, nc):
                over_c[k, i, l].wait_recv()
                total += got_c[k, i, l - 1].astype(wide)
            sum_c[k, i] = total.astype(jnp.bfloat16)
        for j in range(1, nx):
            over_x[k, j] = send(
                sum_c.at[k, lax.rem(x + j, nx)],
                got_x.at[k, j - 1],
                plan.device(plan.shifted(here, "x", j)),
                x_s.at[k, j],
                x_r.at[k, j],
            )

    def fold_x(k):
        total = sum_c[k, x].astype(wide)
        for j in range(1, nx):
            over_x[k, j].wait_recv()
            total += got_x[k, j - 1].astype(wide)
        if k == 0:
            mid_ref[...] += total
            return
        sum_x[k - 1] = total.astype(jnp.bfloat16)
        back[k] = send(
            sum_x.at[k - 1],
            got_z.at[k - 1],
            plan.device(plan.shifted(here, "z", -k)),
            z_s.at[k],
            z_r.at[k],
        )

    for k in range(nz):
        hn.relay_on(k)
        if k + 1 < nz:
            hn.relay(k + 1)
        hn.landed(k)
        feed(k)
        if k:
            fold_x(k - 1)
        fold_c(k)
    fold_x(nz - 1)
    total = mid_ref[...]
    for k in range(1, nz):
        back[k].wait_recv()
        total += got_z[k - 1].astype(wide)
    o_ref[...] = total.astype(jnp.bfloat16)
    kv.finish()
    hn.finish()
    for copies in (over_z, over_r, over_c, over_x, back):
        for copy in copies.values():
            copy.wait_send()
    for copy in swaps:
        copy.wait_send()


def front(plan, heads, part, kv, qp, qr, wk, wv, wo, resid, gain, gate, up, down, ident):
    nz, nr, nx, nc, tp = plan.z, plan.r, plan.x, plan.c, plan.tp
    share, width = resid.shape
    tok = qp.shape[0]
    dma = pltpu.SemaphoreType.DMA
    vmem = pl.BlockSpec(memory_space=pltpu.VMEM)

    def sems(a, b, c):
        return [dma((a,)), dma((a,)), dma((a, b)), dma((a, b)), dma((a, b, c)), dma((a, b, c))]

    bf = jnp.bfloat16
    narrow = down.shape[1]
    downs = (part, plan.sp * narrow) if narrow % 128 == 0 else (plan.sp, part, narrow)
    return pl.pallas_call(
        functools.partial(front_body, plan, heads, part),
        out_shape=jax.ShapeDtypeStruct((share, width), bf),
        in_specs=[vmem] * 11,
        out_specs=vmem,
        scratch_shapes=[
            pltpu.VMEM((share, width), jnp.float32),
            pltpu.VMEM((nz * tp, share, width), bf),
            pltpu.VMEM((plan.sp * gate.shape[0], 2 * part), bf),
            pltpu.VMEM(downs, bf),
            pltpu.VMEM((nz * nr * nc,) + kv.shape, bf),
            pltpu.VMEM((tok, heads * VDIM), bf),
            pltpu.VMEM((tp, share, width), bf),
            pltpu.VMEM((tp, share, width), bf),
            pltpu.VMEM((share, width), bf),
            pltpu.VMEM((nz, nx, nc, share, width), bf),
            pltpu.VMEM((nz, nx, max(nc - 1, 1), share, width), bf),
            pltpu.VMEM((nz, nx, share, width), bf),
            pltpu.VMEM((nz, max(nx - 1, 1), share, width), bf),
            pltpu.VMEM((max(nz - 1, 1), share, width), bf),
            pltpu.VMEM((max(nz - 1, 1), share, width), bf),
            *sems(nz, nr, nc),
            *sems(nz, nx, nc),
            dma((3, nz)),
            dma((3, nz)),
            dma((3, nz, nr)),
            dma((3, nz, nr)),
            dma((tp,)),
            dma((tp,)),
            dma((nz, nx, nc)),
            dma((nz, nx, nc)),
            dma((nz, nx)),
            dma((nz, nx)),
            dma((nz,)),
            dma((nz,)),
            dma((5,)),
        ],
        compiler_params=pltpu.CompilerParams(
            collective_id=ident, has_side_effects=True, vmem_limit_bytes=62 * 1024 * 1024
        ),
    )(kv, qp, qr, wk, wv, wo, resid, gain, gate, up, down)


def shards(
    plan,
    resid_in,
    query_latent,
    kv_latent,
    rotary_key,
    query_gain,
    kv_gain,
    w_query_plain,
    w_query_rotary,
    w_key_plain,
    w_value,
    w_output,
    ffn_gain,
    w_gate,
    w_up,
    w_down,
):
    tok = resid_in.shape[0]
    heads_dev = w_query_plain.shape[1] // NOPE
    nz = plan.z
    hidden_dev = w_gate.shape[1]
    part = min(-(-hidden_dev // (nz * 128)) * 128, hidden_dev)

    offset = lax.axis_index("sp") * tok
    position = (offset + jnp.arange(tok, dtype=jnp.int32)).astype(jnp.float32)
    freq = 10000.0 ** (-jnp.arange(0, ROPE, 2, dtype=jnp.float32) / ROPE)
    angle = position[:, None] * freq[None, :]
    cosine = jnp.cos(angle)
    sine = jnp.sin(angle)
    kv_norm = normed(kv_latent, kv_gain).astype(jnp.bfloat16)
    key_rot = rotate(rotary_key.astype(jnp.float32), cosine, sine).astype(jnp.bfloat16)
    piece = tok // plan.c
    packed = lax.dynamic_slice_in_dim(
        jnp.concatenate([kv_norm, key_rot], axis=1),
        lax.rem(lax.axis_index("tp"), plan.c) * piece,
        piece,
        0,
    )
    q_norm = normed(query_latent, query_gain).astype(jnp.bfloat16)
    q_plain = (
        jnp.dot(q_norm, w_query_plain, preferred_element_type=jnp.float32)
        .astype(jnp.bfloat16)
    )
    q_raw = jnp.dot(q_norm, w_query_rotary, preferred_element_type=jnp.float32).reshape(
        tok, heads_dev, ROPE
    )
    q_rot = rotate(q_raw, cosine[:, None, :], sine[:, None, :]).astype(jnp.bfloat16)
    share = tok // plan.tp
    own_start = lax.axis_index("tp") * share
    return front(
        plan,
        heads_dev,
        part,
        packed,
        q_plain,
        jnp.transpose(q_rot, (1, 0, 2)),
        w_key_plain,
        w_value,
        w_output,
        lax.dynamic_slice_in_dim(resid_in, own_start, share, 0),
        ffn_gain[None, :],
        w_gate,
        w_up,
        w_down,
        1,
    )


def solution(mesh):
    plan = Plan(mesh.shape["sp"], mesh.shape["tp"])
    return jax.shard_map(
        functools.partial(shards, plan),
        mesh=mesh,
        in_specs=(
            P("sp", None),
            P("sp", None),
            P("sp", None),
            P("sp", None),
            P(),
            P(),
            P(None, "tp"),
            P(None, "tp"),
            P(None, "tp"),
            P(None, "tp"),
            P("tp", None),
            P(),
            P("sp", "tp"),
            P("sp", "tp"),
            P("tp", "sp"),
        ),
        out_specs=P(("sp", "tp"), None),
        check_vma=False,
    )
```
